32 devices in a mesh: kv: 8 (over z, y), tp: 4 (over x, core).
Axes of the slice: x: 2, y: 2, z: 4, core: 2. Of those that a mesh axis runs over, the one named last changes fastest.
Arguments:
- stream: bfloat16 [32, 4096], P(None, ('kv', 'tp')), may hold values from -60 to 60
- memory_state: float32 [32, 32, 128, 128], P('kv', 'tp'), may hold values from -3 to 3
- attn_gain: float32 [4096], P('kv'), may hold values from 0.1 to 1.9
- query_weight: bfloat16 [4096, 4096], P('kv', 'tp'), may hold values from -0.09375 to 0.09375
- key_weight: bfloat16 [4096, 4096], P('kv', 'tp'), may hold values from -0.09375 to 0.09375
- value_weight: bfloat16 [4096, 4096], P('kv', 'tp'), may hold values from -0.09375 to 0.09375
- outgate_weight: bfloat16 [4096, 4096], P('kv', 'tp'), may hold values from -0.09375 to 0.09375
- beta_weight: bfloat16 [4096, 32], P('kv', 'tp'), may hold values from -0.09375 to 0.09375
- decay_weight: bfloat16 [4096, 32], P('kv', 'tp'), may hold values from -0.09375 to 0.09375
- decay_log: float32 [32], P('tp'), may hold values from -4 to 1
- decay_shift: float32 [32], P('tp'), may hold values from -3 to 3
- head_gain: float32 [128], replicated, may hold values from 0.1 to 1.9
- output_weight: bfloat16 [4096, 4096], P('tp', 'kv'), may hold values from -0.09375 to 0.09375
- mixer_gain: float32 [4096], P('kv'), may hold values from 0.1 to 1.9
- up_weight: bfloat16 [4096, 16384], P('kv', 'tp'), may hold values from -0.09375 to 0.09375
- down_weight: bfloat16 [16384, 4096], P('tp', 'kv'), may hold values from -0.046875 to 0.046875
Outputs:
- layer_out: bfloat16 [32, 4096], P(None, ('kv', 'tp'))
- memory_next: float32 [32, 32, 128, 128], P('kv', 'tp')
The draws below stay inside these ranges and needn't reach their ends.
All inputs are finite; a program needn't handle non-finite values.
Results may differ from the reference program's by a relative error of at most 0.025.
Values may be sent and summed in bfloat16 or wider, within the bound.
A program may use at most 64 MiB of HBM per device.

```python
import math
import jax
import jax.numpy as jnp
from jax import lax

D = 4096
HEADS = 32
HEAD_DIM = 128
FF = 16384
SEQ_DEV = 4
BATCH = 32
VAL = 4096


def draw_stream(key, part):
    keys = jax.random.split(key, 3)
    columns = jnp.arange(D, dtype=jnp.float32) / D
    base = jnp.clip(jax.random.normal(keys[0], (BATCH, D), jnp.float32), -5.0, 5.0)
    rising = jnp.exp(math.log(3.0) * columns)
    rising = rising / jnp.mean(rising)
    column_scale = rising * jax.random.uniform(keys[1], (D,), jnp.float32, 0.6, 1.4)
    row_scale = jnp.exp(jax.random.uniform(keys[2], (BATCH, 1), jnp.float32, math.log(0.3), math.log(3.0)))
    return (base * column_scale[None, :] * row_scale).astype(jnp.bfloat16)


def shard_levels(own_key, dims, shards, least, largest):
    loudness, own = 1.0, jax.random.fold_in(own_key, 6)
    for dim, blocks in shards:
        draws = jnp.exp(jax.random.uniform(jax.random.fold_in(own, dim), (blocks,), jnp.float32, least / len(shards), largest / len(shards)))
        loudness = loudness * jnp.repeat(draws, dims[dim] // blocks).reshape([-1 if axis == dim else 1 for axis in range(len(dims))])
    return loudness


def centred(own_key, dims, width, limit, cuts=(), kind=jnp.bfloat16):
    drawn = jax.random.normal(own_key, dims, jnp.float32) * width
    if len(cuts) > 0:
        drawn = shard_levels(own_key, dims, cuts, -0.22, 0.18) * drawn
    return jnp.clip(drawn, min=-limit, max=limit).astype(kind)


def setup_inputs(seed: int = 0) -> dict:
    streams_of = jax.random.split(jax.random.key(seed), 17)
    stream = draw_stream(jax.random.fold_in(streams_of[16], 71), 0)
    memory_state = centred(streams_of[1], (BATCH, HEADS, HEAD_DIM, HEAD_DIM), 0.5, 3.0, ((0, 8), (1, 4)), jnp.float32)
    attn_gain = jnp.clip(1.0 + 0.18 * jax.random.normal(streams_of[2], (D,), jnp.float32), 0.1, 1.9)
    query_weight = centred(streams_of[3], (D, VAL), D ** -0.5, 0.09375, ((0, 8), (1, 4)))
    key_weight = centred(streams_of[4], (D, VAL), D ** -0.5, 0.09375, ((0, 8), (1, 4)))
    value_weight = centred(streams_of[5], (D, VAL), D ** -0.5, 0.09375, ((0, 8), (1, 4)))
    outgate_weight = centred(streams_of[6], (D, VAL), D ** -0.5, 0.09375, ((0, 8), (1, 4)))
    beta_weight = centred(streams_of[7], (D, HEADS), D ** -0.5, 0.09375, ((0, 8), (1, 4)))
    decay_weight = centred(streams_of[8], (D, HEADS), D ** -0.5, 0.09375, ((0, 8), (1, 4)))
    decay_log = jnp.clip(-4.0 + 5.0 * jax.random.uniform(streams_of[9], (HEADS,), jnp.float32) ** shard_levels(streams_of[9], (HEADS,), ((0, 4),), -0.2, 0.2), -4.0, 1.0)
    decay_shift = centred(streams_of[10], (HEADS,), 1.0, 3.0, ((0, 4),), jnp.float32)
    head_gain = jnp.clip(1.0 + 0.18 * jax.random.normal(streams_of[11], (HEAD_DIM,), jnp.float32), 0.1, 1.9)
    output_weight = centred(streams_of[12], (VAL, D), VAL ** -0.5, 0.09375, ((0, 4), (1, 8)))
    mixer_gain = jnp.clip(1.0 + 0.18 * jax.random.normal(streams_of[13], (D,), jnp.float32), 0.1, 1.9)
    up_weight = centred(streams_of[14], (D, FF), D ** -0.5, 0.09375, ((0, 8), (1, 4)))
    down_weight = centred(streams_of[15], (FF, D), FF ** -0.5, 0.046875, ((0, 4), (1, 8)))
    return dict(stream=stream, memory_state=memory_state, attn_gain=attn_gain, query_weight=query_weight, key_weight=key_weight, value_weight=value_weight, outgate_weight=outgate_weight, beta_weight=beta_weight, decay_weight=decay_weight, decay_log=decay_log, decay_shift=decay_shift, head_gain=head_gain, output_weight=output_weight, mixer_gain=mixer_gain, up_weight=up_weight, down_weight=down_weight)


epsilon = 1e-06

def normed_rows(stream, gain_vec):
    widened = stream.astype(jnp.float32)
    factor = lax.rsqrt(lax.optimization_barrier(jnp.sum(widened * widened, axis=1)) / D + epsilon)
    scaled = (widened * gain_vec.astype(jnp.float32)).astype(jnp.bfloat16)
    return (scaled, factor[:, None])

def unit_rows(values):
    return values * lax.rsqrt(lax.optimization_barrier(jnp.sum(values * values, axis=-1, keepdims=True)) + epsilon)

def head_output(memory_state, query_sum, key_sum, value_sum, gate_sum, beta_sum, decay_sum, decay_log, decay_shift, head_gain):
    row_count = query_sum.shape[0]
    head_count = beta_sum.shape[1]

    def to_heads(values):
        return values.reshape(row_count, head_count, HEAD_DIM)
    query_heads = unit_rows(jax.nn.silu(to_heads(query_sum))) * HEAD_DIM ** (-0.5)
    key_heads = unit_rows(jax.nn.silu(to_heads(key_sum)))
    value_heads = jax.nn.silu(to_heads(value_sum))
    beta_heads = jax.nn.sigmoid(beta_sum)
    decay_heads = jnp.exp(-jnp.exp(decay_log) * jax.nn.softplus(decay_sum + decay_shift))
    kept_state = memory_state * decay_heads[:, :, None, None]
    recalled = jnp.einsum('bhkv,bhk->bhv', kept_state, key_heads)
    correction = beta_heads[:, :, None] * (value_heads - recalled)
    memory_next = kept_state + key_heads[:, :, :, None] * correction[:, :, None, :]
    readout = jnp.einsum('bhkv,bhk->bhv', memory_next, query_heads)
    normed = readout * lax.rsqrt(lax.optimization_barrier(jnp.mean(readout * readout, axis=-1, keepdims=True)) + epsilon)
    gated = normed * head_gain.astype(jnp.float32) * jax.nn.silu(to_heads(gate_sum))
    return (gated.reshape(row_count, head_count * HEAD_DIM).astype(jnp.bfloat16), memory_next)

def reference(stream, memory_state, attn_gain, query_weight, key_weight, value_weight, outgate_weight, beta_weight, decay_weight, decay_log, decay_shift, head_gain, output_weight, mixer_gain, up_weight, down_weight):
    batch_rows = stream.shape[0]
    scaled, factor = normed_rows(stream, attn_gain)

    def project(weight):
        return jnp.dot(scaled, weight, preferred_element_type=jnp.float32) * factor
    sums = tuple((project(weight) for weight in (query_weight, key_weight, value_weight, outgate_weight, beta_weight, decay_weight)))
    groups = batch_rows // SEQ_DEV

    def regroup(values):
        return values.reshape((groups, SEQ_DEV) + values.shape[1:])

    def one_group(inputs):
        return head_output(*inputs, decay_log, decay_shift, head_gain)
    heads_out, memory_next = lax.map(one_group, (regroup(memory_state),) + tuple((regroup(values) for values in sums)))
    heads_out = heads_out.reshape(batch_rows, heads_out.shape[-1])
    memory_next = memory_next.reshape(memory_state.shape)
    attn = jnp.dot(heads_out, output_weight, preferred_element_type=jnp.float32)
    middle = (stream.astype(jnp.float32) + attn).astype(jnp.bfloat16)
    scaled_mix, factor_mix = normed_rows(middle, mixer_gain)
    up_values = jnp.dot(scaled_mix, up_weight, preferred_element_type=jnp.float32) * factor_mix
    hidden = jnp.square(jax.nn.relu(up_values)).astype(jnp.bfloat16)
    mixer = jnp.dot(hidden, down_weight, preferred_element_type=jnp.float32)
    layer_out = (middle.astype(jnp.float32) + mixer).astype(jnp.bfloat16)
    return (layer_out, memory_next)
```

```python
import functools

import jax
import jax.numpy as jnp
from jax import lax
from jax.experimental import pallas as pl
from jax.experimental.pallas import tpu as pltpu
from jax.sharding import PartitionSpec as P

MESH = pl.DeviceIdType.MESH
F32 = jnp.float32
BF16 = jnp.bfloat16
epsilon = 1e-06
LANES = 128
CHUNKS = 2


def silu(x):
    return x * jax.nn.sigmoid(x)


def layer_kernel(
    nkv, ntp,
    stream_h, state_h, again_h, qw_h, kw_h, vw_h, gw_h, bw_h, dw_h, dlog_h, dshift_h, hgain_h,
    ow_h, mgain_h, uw_h, dn_h,
    out_v, next_h,
    stream_v, state_v, again_v, proj_v, bw_v, dw_v, dlog_v, dshift_v, hgain_v, ow_v, mgain_v, uw_v, dn_v,
    next_v, sbuf, psend, precv, bsend, brecv, y_v, dec_v, beta_v, ro_v, hbuf, abuf, mid_v, qbuf,
    usend, urecv, hidbuf, dsend, drecv,
    lsem, s_send, s_recv, p_send, p_recv, b_send, b_recv, h_send, h_recv, a_send, a_recv,
    q_send, q_recv, u_send, u_recv, f_send, f_recv, d_send, d_recv,
):
    kv = lax.axis_index("kv")
    tp = lax.axis_index("tp")
    rows, width = stream_v.shape
    depth = again_v.shape[1]
    model = depth * nkv
    vals = proj_v.shape[2]
    seqs, heads, hd, _ = state_v.shape
    cw = vals // CHUNKS

    def kv_to(d):
        return lax.rem(kv + d, nkv)

    def kv_from(d):
        return lax.rem(kv + nkv - d, nkv)

    def tp_to(d):
        return lax.rem(tp + d, ntp)

    def tp_from(d):
        return lax.rem(tp + ntp - d, ntp)

    pending = []

    def send(src, dst, ssem, rsem, axis, peer):
        copy = pltpu.make_async_remote_copy(
            src_ref=src, dst_ref=dst, send_sem=ssem, recv_sem=rsem,
            device_id={axis: peer}, device_id_type=MESH,
        )
        copy.start()
        pending.append(copy)
        return copy

    used = [0]

    def load(src, dst):
        copy = pltpu.make_async_copy(src, dst, lsem.at[used[0]])
        used[0] += 1
        copy.start()
        return copy

    c_stream = load(stream_h, stream_v)
    c_again = load(again_h, again_v)
    c_small = [
        load(a, b)
        for a, b in ((bw_h, bw_v), (dw_h, dw_v), (dlog_h, dlog_v), (dshift_h, dshift_v), (hgain_h, hgain_v), (mgain_h, mgain_v))
    ]
    c_proj = []
    for c in range(CHUNKS):
        cols = pl.ds(c * cw, cw)
        c_proj.append([load(w.at[:, cols], proj_v.at[t, :, cols]) for t, w in enumerate((qw_h, kw_h, vw_h, gw_h))])
    c_state = load(state_h, state_v)

    barrier = pltpu.get_barrier_semaphore()
    for d in range(1, nkv):
        pl.semaphore_signal(barrier, inc=1, device_id={"kv": kv_to(d)}, device_id_type=MESH)
    for d in range(1, ntp):
        pl.semaphore_signal(barrier, inc=1, device_id={"tp": tp_to(d)}, device_id_type=MESH)
    pl.semaphore_wait(barrier, nkv + ntp - 2)

    c_stream.wait()
    for d in range(1, ntp):
        send(stream_v, sbuf.at[tp], s_send.at[d], s_recv.at[d], "tp", tp_to(d))
    sbuf[tp] = stream_v[...]
    c_again.wait()
    for copy in c_small:
        copy.wait()
    for d in range(1, ntp):
        pltpu.make_async_remote_copy(
            src_ref=stream_v, dst_ref=sbuf.at[tp_from(d)], send_sem=s_send.at[d], recv_sem=s_recv.at[d],
            device_id={"tp": tp_to(d)}, device_id_type=MESH,
        ).wait_recv()
    full = jnp.concatenate([sbuf[s].astype(F32) for s in range(ntp)], axis=1)
    squares = jnp.sum(full * full, axis=1, keepdims=True)
    scaled = (full * again_v[...]).astype(BF16)

    beta_part = jnp.dot(scaled, bw_v[...], preferred_element_type=F32)
    decay_part = jnp.dot(scaled, dw_v[...], preferred_element_type=F32)
    square_part = jnp.broadcast_to(squares, (rows, heads))
    for j in range(nkv):
        part = slice(j * seqs, (j + 1) * seqs)
        bsend[j] = jnp.concatenate([beta_part[part], decay_part[part], square_part[part], square_part[part]], axis=0)
    b_copies = [
        send(bsend.at[kv_to(d)], brecv.at[d], b_send.at[d], b_recv.at[d], "kv", kv_to(d)) for d in range(1, nkv)
    ]
    p_copies = []
    for c in range(CHUNKS):
        for copy in c_proj[c]:
            copy.wait()
        parts = [
            jnp.dot(scaled, proj_v[t, :, c * cw : (c + 1) * cw], preferred_element_type=F32) for t in range(4)
        ]
        for j in range(nkv):
            part = slice(j * seqs, (j + 1) * seqs)
            psend[c, j] = jnp.concatenate([p[part] for p in parts], axis=0).astype(BF16)
        p_copies.append([
            send(psend.at[c, kv_to(d)], precv.at[c, d], p_send.at[c, d], p_recv.at[c, d], "kv", kv_to(d))
            for d in range(1, nkv)
        ])

    c_out = load(ow_h, ow_v)
    c_up = load(uw_h, uw_v)
    c_down = load(dn_h, dn_v)

    small = bsend[kv]
    for d in range(1, nkv):
        b_copies[d - 1].wait_recv()
        small = small + brecv[d]
    factor = lax.rsqrt(small[2 * seqs : 3 * seqs, 0:1] / model + epsilon)
    beta = jax.nn.sigmoid(small[0:seqs] * factor)
    decay_in = small[seqs : 2 * seqs] * factor + dshift_v[...]
    decay = jnp.exp(-jnp.exp(dlog_v[...]) * jax.nn.softplus(decay_in))
    for h in range(heads):
        dec_v[h * seqs : (h + 1) * seqs, :] = jnp.broadcast_to(decay[:, h : h + 1], (seqs, hd))
        beta_v[h * seqs : (h + 1) * seqs, :] = jnp.broadcast_to(beta[:, h : h + 1], (seqs, hd))
    kinds = 4 * seqs
    factor_rows = jnp.concatenate([factor] * 4, axis=0)
    kind = lax.broadcasted_iota(jnp.int32, (kinds, 1), 0) // seqs
    c_state.wait()
    groups = kinds // seqs
    per_group = heads // groups
    heads_chunk = cw // hd
    for c in range(CHUNKS):
        total = psend[c, kv].astype(F32)
        for d in range(1, nkv):
            p_copies[c][d - 1].wait_recv()
            total = total + precv[c, d].astype(F32)
        tall = []
        for hh in range(heads_chunk):
            x = silu(total[:, hh * hd : (hh + 1) * hd] * factor_rows)
            norm = lax.rsqrt(jnp.sum(x * x, axis=1, keepdims=True) + epsilon)
            scale = jnp.where(kind == 0, norm * hd ** (-0.5), jnp.where(kind == 1, norm, 1.0))
            tall.append(x * scale)
        y = jnp.concatenate(tall, axis=0)
        y_v[c] = y
        y_t = y.T
        for hh in range(heads_chunk):
            h = c * heads_chunk + hh
            for b in range(seqs):
                row = h * seqs + b
                base = hh * kinds + b
                q_col = y_t[:, base : base + 1]
                k_col = y_t[:, base + seqs : base + seqs + 1]
                kept = state_v[b, h] * dec_v[row : row + 1, :]
                recalled = jnp.sum(kept * k_col, axis=0, keepdims=True)
                value = y_v[c, base + 2 * seqs : base + 2 * seqs + 1, :]
                correction = beta_v[row : row + 1, :] * (value - recalled)
                after = kept + k_col * correction
                next_v[b, h] = after
                group, place = h // per_group, h % per_group
                at = place * kinds + group * seqs + b
                ro_v[at : at + 1, :] = jnp.sum(after * q_col, axis=0, keepdims=True)
    c_next = pltpu.make_async_copy(next_v, next_h, lsem.at[used[0]])
    c_next.start()
    used[0] += 1

    pieces = []
    for place in range(per_group):
        readout = ro_v[place * kinds : (place + 1) * kinds, :]
        gates = []
        for group in range(groups):
            h = group * per_group + place
            base = (h % heads_chunk) * kinds + 3 * seqs
            gates.append(y_v[h // heads_chunk, base : base + seqs, :])
        gate = jnp.concatenate(gates, axis=0)
        normed = readout * lax.rsqrt(jnp.mean(readout * readout, axis=1, keepdims=True) + epsilon)
        pieces.append(normed * hgain_v[...] * gate)
    hbuf[kv] = jnp.concatenate(pieces, axis=1).astype(BF16)
    for d in range(1, nkv):
        send(hbuf.at[kv], hbuf.at[kv], h_send.at[d], h_recv.at[d], "kv", kv_to(d))
    c_out.wait()
    for d in range(1, nkv):
        pltpu.make_async_remote_copy(
            src_ref=hbuf.at[kv], dst_ref=hbuf.at[kv_from(d)], send_sem=h_send.at[d], recv_sem=h_recv.at[d],
            device_id={"kv": kv_to(d)}, device_id_type=MESH,
        ).wait_recv()
    blocks = [hbuf[s].astype(F32) for s in range(nkv)]
    ordered = jnp.concatenate(
        [
            jnp.concatenate([block[g * seqs : (g + 1) * seqs] for block in blocks], axis=0)
            for g in range(groups)
        ],
        axis=1,
    ).astype(BF16)
    attn_part = jnp.dot(ordered, ow_v[...], preferred_element_type=F32)

    abuf[tp] = attn_part.astype(BF16)
    for d in range(1, ntp):
        send(abuf.at[tp], abuf.at[tp], a_send.at[d], a_recv.at[d], "tp", tp_to(d))
    for d in range(1, ntp):
        pltpu.make_async_remote_copy(
            src_ref=abuf.at[tp], dst_ref=abuf.at[tp_from(d)], send_sem=a_send.at[d], recv_sem=a_recv.at[d],
            device_id={"tp": tp_to(d)}, device_id_type=MESH,
        ).wait_recv()
    attn = abuf[0].astype(F32)
    for s in range(1, ntp):
        attn = attn + abuf[s].astype(F32)
    stream_all = jnp.concatenate([sbuf[s].astype(F32) for s in range(ntp)], axis=1)
    middle = (stream_all + attn).astype(BF16).astype(F32)
    for s in range(ntp):
        mid_v[s] = middle[:, s * width : (s + 1) * width]
    square_mix = jnp.sum(middle * middle, axis=1, keepdims=True)
    lanes = qbuf.shape[2]
    diagonal = lax.broadcasted_iota(jnp.int32, (rows, lanes), 0) == lax.broadcasted_iota(jnp.int32, (rows, lanes), 1)
    flat = jnp.sum(jnp.where(diagonal, square_mix, 0.0), axis=0, keepdims=True)
    qbuf[0] = jnp.broadcast_to(flat, qbuf.shape[1:])
    q_copies = [
        send(qbuf.at[0], qbuf.at[d], q_send.at[d], q_recv.at[d], "kv", kv_to(d)) for d in range(1, nkv)
    ]
    mixed = (middle * mgain_v[...]).astype(BF16)

    c_up.wait()
    uw = uw_v.shape[1] // nkv
    u_copies = []
    if uw % LANES == 0:
        for d in range(1, nkv + 1):
            peer = kv_to(d)
            cols = pl.ds(pl.multiple_of(peer * uw, LANES), uw)
            part = jnp.dot(mixed, uw_v[:, cols], preferred_element_type=F32)
            if d < nkv:
                usend[d] = part.astype(BF16)
                u_copies.append(send(usend.at[d], urecv.at[d], u_send.at[d], u_recv.at[d], "kv", peer))
            else:
                own = part
    else:
        part = jnp.dot(mixed, uw_v[...], preferred_element_type=F32).astype(BF16)
        for j in range(nkv):
            usend[j] = part[:, j * uw : (j + 1) * uw]
        for d in range(1, nkv):
            u_copies.append(send(usend.at[kv_to(d)], urecv.at[d], u_send.at[d], u_recv.at[d], "kv", kv_to(d)))
        own = usend[kv].astype(F32)
    for d in range(1, nkv):
        q_copies[d - 1].wait_recv()
    total_flat = jnp.sum(qbuf[...], axis=0)[0:1, :]
    total_mix = jnp.sum(jnp.where(diagonal, total_flat, 0.0), axis=1, keepdims=True)
    factor_mix = lax.rsqrt(total_mix / model + epsilon)
    for d in range(1, nkv):
        u_copies[d - 1].wait_recv()
        own = own + urecv[d].astype(F32)
    hidden = jnp.square(jnp.maximum(own * factor_mix, 0.0)).astype(BF16)
    hidbuf[0] = hidden
    f_copies = [
        send(hidbuf.at[0], hidbuf.at[d], f_send.at[d], f_recv.at[d], "kv", kv_to(d)) for d in range(1, nkv)
    ]
    c_down.wait()
    down = None
    for d in range(nkv):
        if d > 0:
            f_copies[d - 1].wait_recv()
        units = pl.ds(pl.multiple_of(kv_from(d) * uw, uw), uw)
        term = jnp.dot(hidbuf[d], dn_v[units, :], preferred_element_type=F32)
        down = term if down is None else down + term
    for s in range(ntp):
        dsend[s] = down[:, s * width : (s + 1) * width].astype(BF16)
    d_copies = [
        send(dsend.at[tp_to(d)], drecv.at[d], d_send.at[d], d_recv.at[d], "tp", tp_to(d)) for d in range(1, ntp)
    ]
    result = dsend[tp].astype(F32)
    for d in range(1, ntp):
        d_copies[d - 1].wait_recv()
        result = result + drecv[d].astype(F32)
    out_v[...] = (mid_v[tp] + result).astype(BF16)
    for copy in pending:
        copy.wait_send()
    c_next.wait()


def layer(nkv, ntp, stream, state, again, qw, kw, vw, gw, bw, dw, dlog, dshift, hgain, ow, mgain, uw, dn):
    rows, width = stream.shape
    depth = again.shape[0]
    vals = qw.shape[1]
    seqs, heads, hd, _ = state.shape
    cw = vals // CHUNKS
    kinds = 4 * seqs
    hidden = uw.shape[1]
    unit = hidden // nkv
    lanes = -(-rows // LANES) * LANES
    cols = ow.shape[1]
    again, mgain, dlog, dshift, hgain = (v.reshape(1, -1) for v in (again, mgain, dlog, dshift, hgain))
    operands = (stream, state, again, qw, kw, vw, gw, bw, dw, dlog, dshift, hgain, ow, mgain, uw, dn)
    vmem, dma = pltpu.VMEM, pltpu.SemaphoreType.DMA

    def like(x):
        return vmem(x.shape, x.dtype)

    scratch = [
        like(stream), like(state), like(again), vmem((4, depth, vals), BF16), like(bw), like(dw), like(dlog),
        like(dshift), like(hgain), like(ow), like(mgain), like(uw), like(dn),
        like(state),
        vmem((ntp, rows, width), BF16),
        vmem((CHUNKS, nkv, kinds, cw), BF16), vmem((CHUNKS, nkv, kinds, cw), BF16),
        vmem((nkv, kinds, heads), F32), vmem((nkv, kinds, heads), F32),
        vmem((CHUNKS, heads // CHUNKS * kinds, hd), F32),
        vmem((heads * seqs, hd), F32), vmem((heads * seqs, hd), F32), vmem((heads * seqs, hd), F32),
        vmem((nkv, kinds, vals * seqs // kinds), BF16),
        vmem((ntp, rows, cols), BF16),
        vmem((ntp, rows, width), F32),
        vmem((nkv, 8, lanes), F32),
        vmem((nkv, rows, unit), BF16), vmem((nkv, rows, unit), BF16), vmem((nkv, rows, unit), BF16),
        vmem((ntp, rows, width), BF16), vmem((ntp, rows, width), BF16),
        dma((8 + 4 * CHUNKS + 5,)),
        dma((ntp,)), dma((ntp,)),
        dma((CHUNKS, nkv)), dma((CHUNKS, nkv)),
        dma((nkv,)), dma((nkv,)), dma((nkv,)), dma((nkv,)),
        dma((ntp,)), dma((ntp,)),
        dma((nkv,)), dma((nkv,)), dma((nkv,)), dma((nkv,)), dma((nkv,)), dma((nkv,)),
        dma((ntp,)), dma((ntp,)),
    ]
    return pl.pallas_call(
        functools.partial(layer_kernel, nkv, ntp),
        out_shape=(
            jax.ShapeDtypeStruct((rows, width), BF16),
            jax.ShapeDtypeStruct(state.shape, state.dtype),
        ),
        in_specs=[pl.BlockSpec(memory_space=pl.ANY)] * len(operands),
        out_specs=(pl.BlockSpec(memory_space=pltpu.VMEM), pl.BlockSpec(memory_space=pl.ANY)),
        scratch_shapes=scratch,
        compiler_params=pltpu.CompilerParams(
            collective_id=0, has_side_effects=True, vmem_limit_bytes=60 * 1024 * 1024
        ),
    )(*operands)


def solution(mesh):
    in_specs = (
        P(None, ("kv", "tp")),
        P("kv", "tp", None, None),
        P("kv"),
        P("kv", "tp"),
        P("kv", "tp"),
        P("kv", "tp"),
        P("kv", "tp"),
        P("kv", "tp"),
        P("kv", "tp"),
        P("tp"),
        P("tp"),
        P(),
        P("tp", "kv"),
        P("kv"),
        P("kv", "tp"),
        P("tp", "kv"),
    )
    out_specs = (P(None, ("kv", "tp")), P("kv", "tp", None, None))
    shards = functools.partial(layer, mesh.shape["kv"], mesh.shape["tp"])
    return jax.shard_map(shards, mesh=mesh, in_specs=in_specs, out_specs=out_specs, check_vma=False)
```

```python
import functools

import jax
import jax.numpy as jnp
from jax import lax
from jax.experimental import pallas as pl
from jax.experimental.pallas import tpu as pltpu
from jax.sharding import PartitionSpec as P

MESH = pl.DeviceIdType.MESH
F32 = jnp.float32
BF16 = jnp.bfloat16
epsilon = 1e-06
LANES = 128
CHUNKS = 2


def silu(x):
    return x * jax.nn.sigmoid(x)


def across(a, b):
    return lax.dot_general(a, b, (((1,), (1,)), ((), ())), preferred_element_type=F32)


def layer_kernel(
    nkv, ntp,
    stream_h, state_h, again_h, qw_h, kw_h, vw_h, gw_h, bw_h, dw_h, dlog_h, dshift_h, hgain_h,
    ow_h, mgain_h, uw_h, dn_h,
    out_v, next_v,
    stream_v, state_v, again_v, proj_v, bw_v, dw_v, dlog_v, dshift_v, hgain_v, ow_v, mgain_v, uw_v, dn_v,
    sbuf, psend, precv, bsend, brecv, y_v, dec_v, beta_v, ro_v, hbuf, abuf, mid_v, qbuf,
    usend, urecv, hidbuf, dsend, drecv,
    lsem, s_send, s_recv, p_send, p_recv, b_send, b_recv, h_send, h_recv, a_send, a_recv,
    q_send, q_recv, u_send, u_recv, f_send, f_recv, d_send, d_recv,
):
    kv = lax.axis_index("kv")
    tp = lax.axis_index("tp")
    rows, width = stream_v.shape
    depth = again_v.shape[1]
    model = depth * nkv
    vals = proj_v.shape[2]
    seqs, heads, hd, _ = state_v.shape
    cw = vals // CHUNKS

    paired = nkv & (nkv - 1) == 0
    far_first = range(nkv - 1, 0, -1)

    def flipped(d):
        peer, bit = kv, 1
        while bit < nkv:
            if d & bit:
                peer = peer + bit * (1 - 2 * ((kv // bit) % 2))
            bit *= 2
        return peer

    def kv_to(d):
        return flipped(d) if paired else lax.rem(kv + d, nkv)

    def kv_from(d):
        return flipped(d) if paired else lax.rem(kv + nkv - d, nkv)

    def tp_to(d):
        return lax.rem(tp + d, ntp)

    def tp_from(d):
        return lax.rem(tp + ntp - d, ntp)

    pending = []

    def send(src, dst, ssem, rsem, axis, peer):
        copy = pltpu.make_async_remote_copy(
            src_ref=src, dst_ref=dst, send_sem=ssem, recv_sem=rsem,
            device_id={axis: peer}, device_id_type=MESH,
        )
        copy.start()
        pending.append(copy)
        return copy

    used = [0]

    def load(src, dst):
        copy = pltpu.make_async_copy(src, dst, lsem.at[used[0]])
        used[0] += 1
        copy.start()
        return copy

    c_stream = load(stream_h, stream_v)
    c_again = load(again_h, again_v)
    c_small = [
        load(a, b)
        for a, b in ((bw_h, bw_v), (dw_h, dw_v), (dlog_h, dlog_v), (dshift_h, dshift_v), (hgain_h, hgain_v), (mgain_h, mgain_v))
    ]
    c_proj = []
    for c in range(CHUNKS):
        cols = pl.ds(c * cw, cw)
        c_proj.append([load(w.at[:, cols], proj_v.at[t, :, cols]) for t, w in enumerate((qw_h, kw_h, vw_h, gw_h))])
    c_state = load(state_h, state_v)

    barrier = pltpu.get_barrier_semaphore()
    for d in range(1, nkv):
        pl.semaphore_signal(barrier, inc=1, device_id={"kv": kv_to(d)}, device_id_type=MESH)
    for d in range(1, ntp):
        pl.semaphore_signal(barrier, inc=1, device_id={"tp": tp_to(d)}, device_id_type=MESH)
    pl.semaphore_wait(barrier, nkv + ntp - 2)

    c_stream.wait()
    for d in range(1, ntp):
        send(stream_v, sbuf.at[tp], s_send.at[d], s_recv.at[d], "tp", tp_to(d))
    sbuf[tp] = stream_v[...]
    c_again.wait()
    for copy in c_small:
        copy.wait()
    for d in range(1, ntp):
        pltpu.make_async_remote_copy(
            src_ref=stream_v, dst_ref=sbuf.at[tp_from(d)], send_sem=s_send.at[d], recv_sem=s_recv.at[d],
            device_id={"tp": tp_to(d)}, device_id_type=MESH,
        ).wait_recv()
    full = jnp.concatenate([sbuf[s].astype(F32) for s in range(ntp)], axis=1)
    squares = jnp.sum(full * full, axis=1, keepdims=True)
    scaled = (full * again_v[...]).astype(BF16)

    beta_part = across(scaled, bw_v[...])
    decay_part = across(scaled, dw_v[...])
    square_part = jnp.broadcast_to(squares, (rows, heads))
    for j in range(nkv):
        part = slice(j * seqs, (j + 1) * seqs)
        bsend[j] = jnp.concatenate([beta_part[part], decay_part[part], square_part[part], square_part[part]], axis=0)
    b_copies = {
        d: send(bsend.at[kv_to(d)], brecv.at[d], b_send.at[d], b_recv.at[d], "kv", kv_to(d)) for d in far_first
    }
    p_copies = []
    for c in range(CHUNKS):
        for copy in c_proj[c]:
            copy.wait()
        parts = [
            jnp.dot(scaled, proj_v[t, :, c * cw : (c + 1) * cw], preferred_element_type=F32) for t in range(4)
        ]
        for j in range(nkv):
            part = slice(j * seqs, (j + 1) * seqs)
            psend[c, j] = jnp.concatenate([p[part] for p in parts], axis=0).astype(BF16)
        p_copies.append({
            d: send(psend.at[c, kv_to(d)], precv.at[c, d], p_send.at[c, d], p_recv.at[c, d], "kv", kv_to(d))
            for d in far_first
        })

    c_out = load(ow_h, ow_v)
    c_up = load(uw_h, uw_v)
    c_down = load(dn_h, dn_v)

    small = bsend[kv]
    for d in range(1, nkv):
        b_copies[d].wait_recv()
        small = small + brecv[d]
    factor = lax.rsqrt(small[2 * seqs : 3 * seqs, 0:1] / model + epsilon)
    beta = jax.nn.sigmoid(small[0:seqs] * factor)
    decay_in = small[seqs : 2 * seqs] * factor + dshift_v[...]
    decay = jnp.exp(-jnp.exp(dlog_v[...]) * jax.nn.softplus(decay_in))
    for h in range(heads):
        dec_v[h * seqs : (h + 1) * seqs, :] = jnp.broadcast_to(decay[:, h : h + 1], (seqs, hd))
        beta_v[h * seqs : (h + 1) * seqs, :] = jnp.broadcast_to(beta[:, h : h + 1], (seqs, hd))
    kinds = 4 * seqs
    factor_rows = jnp.concatenate([factor] * 4, axis=0)
    kind = lax.broadcasted_iota(jnp.int32, (kinds, 1), 0) // seqs
    c_state.wait()
    groups = kinds // seqs
    per_group = heads // groups
    heads_chunk = cw // hd
    for c in range(CHUNKS):
        total = psend[c, kv].astype(F32)
        for d in range(1, nkv):
            p_copies[c][d].wait_recv()
            total = total + precv[c, d].astype(F32)
        tall = []
        for hh in range(heads_chunk):
            x = silu(total[:, hh * hd : (hh + 1) * hd] * factor_rows)
            norm = lax.rsqrt(jnp.sum(x * x, axis=1, keepdims=True) + epsilon)
            scale = jnp.where(kind == 0, norm * hd ** (-0.5), jnp.where(kind == 1, norm, 1.0))
            tall.append(x * scale)
        y = jnp.concatenate(tall, axis=0)
        y_v[c] = y
        y_t = y.T
        for hh in range(heads_chunk):
            h = c * heads_chunk + hh
            for b in range(seqs):
                row = h * seqs + b
                base = hh * kinds + b
                q_col = y_t[:, base : base + 1]
                k_col = y_t[:, base + seqs : base + seqs + 1]
                kept = state_v[b, h] * dec_v[row : row + 1, :]
                recalled = jnp.sum(kept * k_col, axis=0, keepdims=True)
                value = y_v[c, base + 2 * seqs : base + 2 * seqs + 1, :]
                correction = beta_v[row : row + 1, :] * (value - recalled)
                after = kept + k_col * correction
                next_v[b, h] = after
                group, place = h // per_group, h % per_group
                at = place * kinds + group * seqs + b
                ro_v[at : at + 1, :] = jnp.sum(after * q_col, axis=0, keepdims=True)

    pieces = []
    for place in range(per_group):
        readout = ro_v[place * kinds : (place + 1) * kinds, :]
        gates = []
        for group in range(groups):
            h = group * per_group + place
            base = (h % heads_chunk) * kinds + 3 * seqs
            gates.append(y_v[h // heads_chunk, base : base + seqs, :])
        gate = jnp.concatenate(gates, axis=0)
        normed = readout * lax.rsqrt(jnp.mean(readout * readout, axis=1, keepdims=True) + epsilon)
        pieces.append(normed * hgain_v[...] * gate)
    hbuf[kv] = jnp.concatenate(pieces, axis=1).astype(BF16)
    for d in far_first:
        send(hbuf.at[kv], hbuf.at[kv], h_send.at[d], h_recv.at[d], "kv", kv_to(d))
    c_out.wait()
    for d in range(1, nkv):
        pltpu.make_async_remote_copy(
            src_ref=hbuf.at[kv], dst_ref=hbuf.at[kv_from(d)], send_sem=h_send.at[d], recv_sem=h_recv.at[d],
            device_id={"kv": kv_to(d)}, device_id_type=MESH,
        ).wait_recv()
    blocks = [hbuf[s].astype(F32) for s in range(nkv)]
    ordered = jnp.concatenate(
        [
            jnp.concatenate([block[g * seqs : (g + 1) * seqs] for block in blocks], axis=0)
            for g in range(groups)
        ],
        axis=1,
    ).astype(BF16)
    attn_part = jnp.dot(ordered, ow_v[...], preferred_element_type=F32)

    abuf[tp] = attn_part.astype(BF16)
    for d in range(1, ntp):
        send(abuf.at[tp], abuf.at[tp], a_send.at[d], a_recv.at[d], "tp", tp_to(d))
    for d in range(1, ntp):
        pltpu.make_async_remote_copy(
            src_ref=abuf.at[tp], dst_ref=abuf.at[tp_from(d)], send_sem=a_send.at[d], recv_sem=a_recv.at[d],
            device_id={"tp": tp_to(d)}, device_id_type=MESH,
        ).wait_recv()
    attn = abuf[0].astype(F32)
    for s in range(1, ntp):
        attn = attn + abuf[s].astype(F32)
    stream_all = jnp.concatenate([sbuf[s].astype(F32) for s in range(ntp)], axis=1)
    middle = (stream_all + attn).astype(BF16).astype(F32)
    for s in range(ntp):
        mid_v[s] = middle[:, s * width : (s + 1) * width]
    square_mix = jnp.sum(middle * middle, axis=1, keepdims=True)
    lanes = qbuf.shape[2]
    diagonal = lax.broadcasted_iota(jnp.int32, (rows, lanes), 0) == lax.broadcasted_iota(jnp.int32, (rows, lanes), 1)
    flat = jnp.sum(jnp.where(diagonal, square_mix, 0.0), axis=0, keepdims=True)
    qbuf[0] = jnp.broadcast_to(flat, qbuf.shape[1:])
    q_copies = {
        d: send(qbuf.at[0], qbuf.at[d], q_send.at[d], q_recv.at[d], "kv", kv_to(d)) for d in far_first
    }
    mixed = (middle * mgain_v[...]).astype(BF16)

    c_up.wait()
    uw = uw_v.shape[1] // nkv
    u_copies = {}
    if uw % LANES == 0:
        for d in (*far_first, 0):
            peer = kv_to(d)
            cols = pl.ds(pl.multiple_of(peer * uw, LANES), uw)
            part = jnp.dot(mixed, uw_v[:, cols], preferred_element_type=F32)
            if d > 0:
                usend[d] = part.astype(BF16)
                u_copies[d] = send(usend.at[d], urecv.at[d], u_send.at[d], u_recv.at[d], "kv", peer)
            else:
                own = part
    else:
        part = jnp.dot(mixed, uw_v[...], preferred_element_type=F32).astype(BF16)
        for j in range(nkv):
            usend[j] = part[:, j * uw : (j + 1) * uw]
        for d in far_first:
            u_copies[d] = send(usend.at[kv_to(d)], urecv.at[d], u_send.at[d], u_recv.at[d], "kv", kv_to(d))
        own = usend[kv].astype(F32)
    for d in range(1, nkv):
        q_copies[d].wait_recv()
    total_flat = jnp.sum(qbuf[...], axis=0)[0:1, :]
    total_mix = jnp.sum(jnp.where(diagonal, total_flat, 0.0), axis=1, keepdims=True)
    factor_mix = lax.rsqrt(total_mix / model + epsilon)
    for d in range(1, nkv):
        u_copies[d].wait_recv()
        own = own + urecv[d].astype(F32)
    hidden = jnp.square(jnp.maximum(own * factor_mix, 0.0)).astype(BF16)
    hidbuf[0] = hidden
    f_copies = {
        d: send(hidbuf.at[0], hidbuf.at[d], f_send.at[d], f_recv.at[d], "kv", kv_to(d)) for d in far_first
    }
    c_down.wait()
    down = None
    for d in range(nkv):
        if d > 0:
            f_copies[d].wait_recv()
        units = pl.ds(pl.multiple_of(kv_from(d) * uw, uw), uw)
        term = jnp.dot(hidbuf[d], dn_v[units, :], preferred_element_type=F32)
        down = term if down is None else down + term
    for s in range(ntp):
        dsend[s] = down[:, s * width : (s + 1) * width].astype(BF16)
    d_copies = [
        send(dsend.at[tp_to(d)], drecv.at[d], d_send.at[d], d_recv.at[d], "tp", tp_to(d)) for d in range(1, ntp)
    ]
    result = dsend[tp].astype(F32)
    for d in range(1, ntp):
        d_copies[d - 1].wait_recv()
        result = result + drecv[d].astype(F32)
    out_v[...] = (mid_v[tp] + result).astype(BF16)
    for copy in pending:
        copy.wait_send()


def layer(nkv, ntp, stream, state, again, qw, kw, vw, gw, bw, dw, dlog, dshift, hgain, ow, mgain, uw, dn):
    rows, width = stream.shape
    depth = again.shape[0]
    vals = qw.shape[1]
    seqs, heads, hd, _ = state.shape
    cw = vals // CHUNKS
    kinds = 4 * seqs
    hidden = uw.shape[1]
    unit = hidden // nkv
    lanes = -(-rows // LANES) * LANES
    cols = ow.shape[1]
    again, mgain, dlog, dshift, hgain = (v.reshape(1, -1) for v in (again, mgain, dlog, dshift, hgain))
    bw, dw = bw.T, dw.T
    operands = (stream, state, again, qw, kw, vw, gw, bw, dw, dlog, dshift, hgain, ow, mgain, uw, dn)
    vmem, dma = pltpu.VMEM, pltpu.SemaphoreType.DMA

    def like(x):
        return vmem(x.shape, x.dtype)

    scratch = [
        like(stream), like(state), like(again), vmem((4, depth, vals), BF16), like(bw), like(dw), like(dlog),
        like(dshift), like(hgain), like(ow), like(mgain), like(uw), like(dn),
        vmem((ntp, rows, width), BF16),
        vmem((CHUNKS, nkv, kinds, cw), BF16), vmem((CHUNKS, nkv, kinds, cw), BF16),
        vmem((nkv, kinds, heads), F32), vmem((nkv, kinds, heads), F32),
        vmem((CHUNKS, heads // CHUNKS * kinds, hd), F32),
        vmem((heads * seqs, hd), F32), vmem((heads * seqs, hd), F32), vmem((heads * seqs, hd), F32),
        vmem((nkv, kinds, vals * seqs // kinds), BF16),
        vmem((ntp, rows, cols), BF16),
        vmem((ntp, rows, width), F32),
        vmem((nkv, 8, lanes), F32),
        vmem((nkv, rows, unit), BF16), vmem((nkv, rows, unit), BF16), vmem((nkv, rows, unit), BF16),
        vmem((ntp, rows, width), BF16), vmem((ntp, rows, width), BF16),
        dma((8 + 4 * CHUNKS + 5,)),
        dma((ntp,)), dma((ntp,)),
        dma((CHUNKS, nkv)), dma((CHUNKS, nkv)),
        dma((nkv,)), dma((nkv,)), dma((nkv,)), dma((nkv,)),
        dma((ntp,)), dma((ntp,)),
        dma((nkv,)), dma((nkv,)), dma((nkv,)), dma((nkv,)), dma((nkv,)), dma((nkv,)),
        dma((ntp,)), dma((ntp,)),
    ]
    return pl.pallas_call(
        functools.partial(layer_kernel, nkv, ntp),
        out_shape=(
            pltpu.VMEM((rows, width), BF16),
            pltpu.VMEM(state.shape, state.dtype),
        ),
        in_specs=[pl.BlockSpec(memory_space=pltpu.HBM)] * len(operands),
        out_specs=(pl.BlockSpec(memory_space=pltpu.VMEM), pl.BlockSpec(memory_space=pltpu.VMEM)),
        scratch_shapes=scratch,
        compiler_params=pltpu.CompilerParams(
            collective_id=0, has_side_effects=True, vmem_limit_bytes=56 * 1024 * 1024
        ),
    )(*operands)


def solution(mesh):
    in_specs = (
        P(None, ("kv", "tp")),
        P("kv", "tp", None, None),
        P("kv"),
        P("kv", "tp"),
        P("kv", "tp"),
        P("kv", "tp"),
        P("kv", "tp"),
        P("kv", "tp"),
        P("kv", "tp"),
        P("tp"),
        P("tp"),
        P(),
        P("tp", "kv"),
        P("kv"),
        P("kv", "tp"),
        P("tp", "kv"),
    )
    out_specs = (P(None, ("kv", "tp")), P("kv", "tp", None, None))
    shards = functools.partial(layer, mesh.shape["kv"], mesh.shape["tp"])
    return jax.shard_map(shards, mesh=mesh, in_specs=in_specs, out_specs=out_specs, check_vma=False)
```
